32 devices in a mesh: ep: 8 (over z, x), tp: 4 (over y, core).
Axes of the slice: x: 2, y: 2, z: 4, core: 2. Of those that a mesh axis runs over, the one named last changes fastest.
Arguments:
- tokens: bfloat16 [384, 2048], P('ep', 'tp'), may hold values from -6 to 6
- conv_state: bfloat16 [384, 3, 1024], P('ep', None, 'tp'), may hold values from -6 to 6
- lru_state: float32 [384, 1024], P('ep', 'tp'), may hold values from -6 to 6
- mix_gain: float32 [2048], replicated, may hold values from 0.1 to 1.9
- input_weight: bfloat16 [2048, 1024], P(None, 'tp'), may hold values from -0.125 to 0.125
- branch_weight: bfloat16 [2048, 1024], P(None, 'tp'), may hold values from -0.125 to 0.125
- conv_taps: float32 [4, 1024], P(None, 'tp'), may hold values from -3 to 3
- conv_bias: float32 [1024], P('tp'), may hold values from -3 to 3
- recur_weight: bfloat16 [8, 128, 128], P('tp'), may hold values from -0.5 to 0.5
- recur_bias: float32 [1024], P('tp'), may hold values from -4 to 4
- inject_weight: bfloat16 [8, 128, 128], P('tp'), may hold values from -0.5 to 0.5
- inject_bias: float32 [1024], P('tp'), may hold values from -4 to 4
- decay_param: float32 [1024], P('tp'), may hold values from -1 to 4
- output_weight: bfloat16 [1024, 2048], P(None, 'tp'), may hold values from -0.1875 to 0.1875
- moe_gain: float32 [2048], replicated, may hold values from 0.1 to 1.9
- route_ids: int32 [384, 2], P('ep'), may hold values from 0 to 7, as said below
- route_logits: float32 [384, 2], P('ep'), may hold values from -6 to 6
- group_weight: float32 [384], P('ep'), may hold values from 0.25 to 1
- expert_gate: bfloat16 [8, 2048, 512], P('ep', None, 'tp'), may hold values from -0.125 to 0.125
- expert_up: bfloat16 [8, 2048, 512], P('ep', None, 'tp'), may hold values from -0.125 to 0.125
- expert_down: bfloat16 [8, 512, 2048], P('ep', 'tp'), may hold values from -0.25 to 0.25
Outputs:
- result: bfloat16 [384, 2048], P('ep', 'tp')
- new_state: float32 [384, 1024], P('ep', 'tp')
- new_conv: bfloat16 [384, 3, 1024], P('ep', None, 'tp')
The draws below stay inside these ranges and needn't reach their ends.
Inputs may be any that keep to these rules, and one draw needn't show every extreme that they name: `route_ids`: each row names 2 different experts of one group of 4 consecutive experts (the group of expert e is e // 4). In each aligned block of 48 rows no expert is named by more than 23 rows, and in every draw some expert is named by exactly 23 rows of every block.
All inputs are finite; a program needn't handle non-finite values.
Results may differ from the reference program's by a relative error of at most 0.013.
Values may be sent and summed in bfloat16 or wider, within the bound.
A program may use at most 64 MiB of HBM per device.

```python
import jax
import jax.numpy as jnp
from jax import lax

D = 2048
LRU_W = 1024
LRU_BLOCKS = 8
BW = 128
TAPS = 4
FF = 512
FF_BLK = 128
PER_GROUP = 4
TOPK = 2
SEQ_GRP = 48
EXPERTS = 8
CAP = 23
BATCH = 384


def draw_route_ids(key, part):
    groups = EXPERTS // PER_GROUP
    reach = PER_GROUP * CAP // TOPK
    slot_total = groups * reach
    group_of = jnp.repeat(jnp.arange(groups, dtype=jnp.int32), reach)
    rank_of = jnp.tile(jnp.arange(reach, dtype=jnp.int32), groups)
    base_key = jax.random.fold_in(key, 17)
    hot_group = jax.random.randint(jax.random.fold_in(base_key, 1), (), 0, groups)
    levels = jax.random.randint(jax.random.fold_in(base_key, 2), (groups,), 0, 4) * 2 ** 16
    column = jnp.arange(groups, dtype=jnp.int32)[:, None] * PER_GROUP + jnp.arange(PER_GROUP, dtype=jnp.int32)[None, :]

    def one_block(block_num, block_key):
        noise_key, perm_key, order_key = jax.random.split(block_key, 3)
        near = (block_num + 1) % EXPERTS
        far = (block_num + EXPERTS // 2) % EXPERTS
        forced = ((group_of == near // PER_GROUP) | (group_of == far // PER_GROUP)) & (rank_of == 0)
        noise = jax.random.randint(noise_key, (slot_total,), 0, 2 ** 16)
        priority = noise + levels[group_of] + jnp.where(group_of == hot_group, 2 ** 18, 0) + jnp.where(forced, 2 ** 19, 0)
        distinct = priority * slot_total + jnp.arange(slot_total, dtype=jnp.int32)
        order = jnp.argsort(-distinct)
        chosen = order[:SEQ_GRP]
        chosen_group = group_of[chosen]
        chosen_rank = rank_of[chosen]
        local_noise = jax.random.randint(perm_key, (groups, PER_GROUP), 0, 2 ** 10) * PER_GROUP + jnp.arange(PER_GROUP, dtype=jnp.int32)[None, :]
        local_noise = jnp.where(column == near, -2, jnp.where(column == far, -1, local_noise))
        arrange = jnp.argsort(local_noise, axis=1).astype(jnp.int32)
        position = (chosen_rank[:, None] * TOPK + jnp.arange(TOPK, dtype=jnp.int32)[None, :]) % PER_GROUP
        local = jnp.take_along_axis(arrange[chosen_group], position, axis=1)
        expert_ids = chosen_group[:, None] * PER_GROUP + local
        shuffle = jax.random.permutation(order_key, SEQ_GRP)
        return expert_ids[shuffle]
    block_keys = jax.random.split(base_key, EXPERTS)
    drawn = jax.vmap(one_block)(jnp.arange(EXPERTS, dtype=jnp.int32), block_keys)
    return drawn.reshape(SEQ_GRP * EXPERTS, TOPK).astype(jnp.int32)


def block_levels(stream_key, extent, cuts, low, top_value):
    level, own = 1.0, jax.random.fold_in(stream_key, 6)
    for axis_at, shards_of in cuts:
        draws = jnp.exp(jax.random.uniform(jax.random.fold_in(own, axis_at), (shards_of,), jnp.float32, low / len(cuts), top_value / len(cuts)))
        level = level * jnp.repeat(draws, extent[axis_at] // shards_of).reshape([-1 if axis == axis_at else 1 for axis in range(len(extent))])
    return level


def centred(key, extent, deviation, most, cuts=(), kind=jnp.bfloat16):
    values = deviation * jax.random.normal(key, extent, jnp.float32)
    if cuts:
        values = values * block_levels(key, extent, cuts, -0.22, 0.18)
    return jnp.clip(values, -most, most).astype(kind)


def setup_inputs(seed: int = 0) -> dict:
    streams_of = jax.random.split(jax.random.key(seed), 22)
    return {
        "tokens": centred(streams_of[0], (BATCH, D), 1.0, 6.0, ((0, 8), (1, 4))),
        "conv_state": centred(streams_of[1], (BATCH, TAPS - 1, LRU_W), 1.0, 6.0, ((0, 8), (2, 4))),
        "lru_state": centred(streams_of[2], (BATCH, LRU_W), 1.0, 6.0, ((0, 8), (1, 4)), jnp.float32),
        "mix_gain": jnp.clip(1.0 + 0.18 * jax.random.normal(streams_of[3], (D,), jnp.float32), 0.1, 1.9),
        "input_weight": centred(streams_of[4], (D, LRU_W), D ** -0.5, 0.125, ((1, 4),)),
        "branch_weight": centred(streams_of[5], (D, LRU_W), D ** -0.5, 0.125, ((1, 4),)),
        "conv_taps": centred(streams_of[6], (TAPS, LRU_W), 0.5, 3.0, ((1, 4),), jnp.float32),
        "conv_bias": centred(streams_of[7], (LRU_W,), 0.5, 3.0, ((0, 4),), jnp.float32),
        "recur_weight": centred(streams_of[8], (LRU_BLOCKS, BW, BW), BW ** -0.5, 0.5, ((0, 4),)),
        "recur_bias": centred(streams_of[9], (LRU_W,), 1.0, 4.0, ((0, 4),), jnp.float32),
        "inject_weight": centred(streams_of[10], (LRU_BLOCKS, BW, BW), BW ** -0.5, 0.5, ((0, 4),)),
        "inject_bias": centred(streams_of[11], (LRU_W,), 1.0, 4.0, ((0, 4),), jnp.float32),
        "decay_param": jnp.clip(-1.0 + 5.0 * jax.random.uniform(streams_of[12], (LRU_W,), jnp.float32) ** block_levels(streams_of[12], (LRU_W,), ((0, 4),), -0.2, 0.2), -1.0, 4.0),
        "output_weight": centred(streams_of[13], (LRU_W, D), LRU_W ** -0.5, 0.1875, ((1, 4),)),
        "moe_gain": jnp.clip(1.0 + 0.18 * jax.random.normal(streams_of[14], (D,), jnp.float32), 0.1, 1.9),
        "route_ids": draw_route_ids(jax.random.fold_in(streams_of[21], 71), 0),
        "route_logits": centred(streams_of[16], (BATCH, TOPK), 1.0, 6.0, ((0, 8),), jnp.float32),
        "group_weight": jnp.clip(0.25 + 0.75 * jax.random.uniform(streams_of[17], (BATCH,), jnp.float32) ** block_levels(streams_of[17], (BATCH,), ((0, 8),), -0.2, 0.2), 0.25, 1.0),
        "expert_gate": centred(streams_of[18], (EXPERTS, D, FF), D ** -0.5, 0.125, ((0, 8), (2, 4))),
        "expert_up": centred(streams_of[19], (EXPERTS, D, FF), D ** -0.5, 0.125, ((0, 8), (2, 4))),
        "expert_down": centred(streams_of[20], (EXPERTS, FF, D), FF ** -0.5, 0.25, ((0, 8), (1, 4))),
    }


EPS = 1e-06
RATE = 8.0

def rms_norm(values, scales):
    wide = values.astype(jnp.float32)
    return wide * lax.rsqrt(lax.optimization_barrier(jnp.mean(wide * wide, axis=-1, keepdims=True)) + EPS) * scales

def block_gate(signal, weight, bias):
    blocks = weight.shape[0]
    grouped = signal.astype(jnp.float32).reshape(signal.shape[0], blocks, -1)
    mixed_out = jnp.einsum('sbi,bij->sbj', grouped, weight.astype(jnp.float32)).reshape(signal.shape[0], -1)
    return jax.nn.sigmoid(mixed_out + bias)

def expert_mix(moe_in, route_ids, route_logits, group_weight, expert_gate, expert_up, expert_down):
    row_total = moe_in.shape[0]
    blocks = row_total // SEQ_GRP
    experts = expert_gate.shape[0]
    flat_ids = route_ids.reshape(blocks, SEQ_GRP * TOPK)
    one_hot = (flat_ids[:, :, None] == jnp.arange(experts, dtype=jnp.int32)[None, None, :]).astype(jnp.int32)
    earlier = jnp.cumsum(one_hot, axis=1) - one_hot
    slot_rank = lax.optimization_barrier(jnp.sum(one_hot * earlier, axis=2))
    block_num = jnp.arange(blocks, dtype=jnp.int32)[:, None]
    slot_index = (flat_ids * (blocks * CAP) + block_num * CAP + slot_rank).reshape(-1).astype(jnp.int32)
    source = jnp.repeat(jnp.arange(row_total, dtype=jnp.int32), TOPK)
    raised = jnp.exp(route_logits)
    route_weight = group_weight[:, None] * raised / lax.optimization_barrier(jnp.sum(raised, axis=1, keepdims=True))
    row_table = jnp.zeros((experts * blocks * CAP,), jnp.int32).at[slot_index].set(source)
    weight_table = jnp.zeros((experts * blocks * CAP,), jnp.float32).at[slot_index].set(route_weight.reshape(-1))
    row_table = row_table.reshape(experts, blocks * CAP)
    weight_table = weight_table.reshape(experts, blocks * CAP)

    def visit(running, members):
        row_index, factor, gate_mat, up_mat, down_mat = members
        picked = jnp.take(moe_in, row_index, axis=0)
        gate_act = jnp.dot(picked, gate_mat, preferred_element_type=jnp.float32)
        up_act = jnp.dot(picked, up_mat, preferred_element_type=jnp.float32)
        hidden = (jax.nn.silu(gate_act) * up_act).astype(jnp.bfloat16)
        summed = jnp.zeros((picked.shape[0], moe_in.shape[1]), jnp.float32)
        for part_num in range(FF // FF_BLK):
            partial_value = jnp.dot(hidden[:, part_num * FF_BLK:(part_num + 1) * FF_BLK], down_mat[part_num * FF_BLK:(part_num + 1) * FF_BLK], preferred_element_type=jnp.float32)
            summed = summed + lax.optimization_barrier(partial_value.astype(jnp.bfloat16)).astype(jnp.float32)
        outcome = lax.optimization_barrier(summed.astype(jnp.bfloat16)).astype(jnp.float32)
        return (running.at[row_index].add(factor[:, None] * outcome), None)
    start_total = jnp.zeros((row_total, moe_in.shape[1]), jnp.float32)
    running, unused = lax.scan(visit, start_total, (row_table, weight_table, expert_gate, expert_up, expert_down))
    return running

def reference(tokens, conv_state, lru_state, mix_gain, input_weight, branch_weight, conv_taps, conv_bias, recur_weight, recur_bias, inject_weight, inject_bias, decay_param, output_weight, moe_gain, route_ids, route_logits, group_weight, expert_gate, expert_up, expert_down):
    normed = rms_norm(tokens, mix_gain).astype(jnp.bfloat16)
    branch_x = jnp.dot(normed, input_weight, preferred_element_type=jnp.float32).astype(jnp.bfloat16)
    branch_g = jnp.dot(normed, branch_weight, preferred_element_type=jnp.float32).astype(jnp.bfloat16)
    window = jnp.concatenate([conv_state, branch_x[:, None, :]], axis=1)
    conv_sum = conv_bias + lax.optimization_barrier(jnp.sum(window.astype(jnp.float32) * conv_taps[None], axis=1))
    conv_out = conv_sum.astype(jnp.bfloat16)
    recur_gate = block_gate(conv_out, recur_weight, recur_bias)
    inject_gate = block_gate(conv_out, inject_weight, inject_bias)
    log_rate = -RATE * recur_gate * jax.nn.softplus(-decay_param)
    new_state = jnp.exp(log_rate) * lru_state + jnp.sqrt(-jnp.expm1(2.0 * log_rate)) * inject_gate * conv_out.astype(jnp.float32)
    mixer_out = (new_state * jax.nn.gelu(branch_g.astype(jnp.float32))).astype(jnp.bfloat16)
    mixed_out = jnp.dot(mixer_out, output_weight, preferred_element_type=jnp.float32)
    stream = (tokens.astype(jnp.float32) + mixed_out).astype(jnp.bfloat16)
    moe_in = rms_norm(stream, moe_gain).astype(jnp.bfloat16)
    routed = expert_mix(moe_in, route_ids, route_logits, group_weight, expert_gate, expert_up, expert_down)
    result = (stream.astype(jnp.float32) + routed).astype(jnp.bfloat16)
    return (result, new_state, window[:, 1:])
```

```python
import functools

import jax
import jax.numpy as jnp
from jax import lax
from jax.experimental import pallas as pl
from jax.experimental.pallas import tpu as pltpu
from jax.sharding import PartitionSpec as P

PER_GROUP = 4
EPS = 1e-06
RATE = 8.0
GROUP = 2
F32 = jnp.float32
BF16 = jnp.bfloat16


def dot(a, b):
    return jnp.dot(a, b, preferred_element_type=F32)


def kernel(
    experts,
    slots,
    tokens,
    conv_pre,
    lru_state,
    mix_gain,
    tap_last,
    recur_weight,
    recur_bias,
    inject_weight,
    inject_bias,
    decay_param,
    moe_gain,
    ids_col,
    ids_row,
    logits,
    group_weight,
    input_hbm,
    branch_hbm,
    output_hbm,
    gate_hbm,
    up_hbm,
    down_hbm,
    result,
    new_state_ref,
    branch_x_ref,
    w_in,
    w_out,
    w_exp,
    w_down,
    tok_all,
    mix_all,
    stream_ref,
    outbox,
    arrived,
    keep_own,
    keep_cross,
    pbox,
    pin,
    xbox,
    xin,
    rbox,
    rin,
    picked,
    w_sem,
    tok_send,
    tok_recv,
    mix_send,
    mix_recv,
    ep_send,
    ep_recv,
    fw_send,
    fw_recv,
    p_send,
    p_recv,
    x_send,
    x_recv,
    r_send,
    r_recv,
):
    e = lax.axis_index("ep")
    t = lax.axis_index("tp")
    rows, quarter = tokens.shape
    width = mix_gain.shape[1]
    chan = lru_state.shape[1]
    chunks = experts // GROUP
    part = t + 1 - 2 * (t % 2)
    cross = (t + 2) % 4
    diag = (part + 2) % 4
    peers = (part, cross, diag)

    def there(member):
        return {"tp": member}

    loads = (
        (input_hbm, w_in.at[:, pl.ds(0, chan)]),
        (branch_hbm, w_in.at[:, pl.ds(chan, chan)]),
        (output_hbm, w_out),
        (gate_hbm, w_exp.at[:, pl.ds(0, gate_hbm.shape[2])]),
        (up_hbm, w_exp.at[:, pl.ds(gate_hbm.shape[2], gate_hbm.shape[2])]),
        (down_hbm, w_down),
    )
    copies = []
    for number, (source, target) in enumerate(loads):
        src = source.at[0] if number >= 3 else source
        copies.append(pltpu.make_async_copy(src, target, w_sem.at[number]))
        copies[-1].start()

    barrier = pltpu.get_barrier_semaphore()
    for member in peers:
        pl.semaphore_signal(barrier, inc=1, device_id=there(member))

    def greet(k, carry):
        pl.semaphore_signal(barrier, inc=1, device_id={"ep": lax.rem(e + k, experts)})
        return carry

    lax.fori_loop(1, experts, greet, 0)
    pl.semaphore_wait(barrier, 3 + experts - 1)

    tok_copies = []
    for number, member in enumerate(peers):
        tok_copies.append(
            pltpu.make_async_remote_copy(
                src_ref=tokens,
                dst_ref=tok_all.at[number],
                send_sem=tok_send.at[number],
                recv_sem=tok_recv.at[number],
                device_id=there(member),
            )
        )
        tok_copies[-1].start()

    first_c, second_c = ids_col[:, 0:1], ids_col[:, 1:2]
    first_r, second_r = ids_row[0:1, :], ids_row[1:2, :]
    row_i = lax.broadcasted_iota(jnp.int32, (rows, rows), 0)
    col_i = lax.broadcasted_iota(jnp.int32, (rows, rows), 1)

    def slot_row(mine):
        same = ((first_c == mine) | (second_c == mine)) & (row_i < col_i)
        rank = jnp.sum(jnp.where(same, 1.0, 0.0), axis=0, keepdims=True)
        return mine * slots + rank.astype(jnp.int32)

    def slot_col(mine):
        same = ((first_r == mine) | (second_r == mine)) & (col_i < row_i)
        rank = jnp.sum(jnp.where(same, 1.0, 0.0), axis=1, keepdims=True)
        return mine * slots + rank.astype(jnp.int32)

    slot_r0, slot_r1 = slot_row(first_r), slot_row(second_r)
    slot_c0, slot_c1 = slot_col(first_c), slot_col(second_c)
    raised = jnp.exp(logits[...])
    route_weight = group_weight[...] * raised / jnp.sum(raised, axis=1, keepdims=True)

    copies[0].wait()
    copies[1].wait()
    total = jnp.zeros((rows, 2 * chan), F32)
    squares = jnp.zeros((rows, 1), F32)
    for number, member in enumerate((t,) + peers):
        if number:
            tok_copies[number - 1].wait_recv()
            wide = tok_all[number - 1].astype(F32)
        else:
            wide = tokens[...].astype(F32)
        span = pl.ds(pl.multiple_of(member * quarter, quarter), quarter)
        squares += jnp.sum(wide * wide, axis=1, keepdims=True)
        total += dot((wide * mix_gain[:, span]).astype(BF16), w_in[span, :])
    total = total * lax.rsqrt(squares / width + EPS)
    branch_x = total[:, :chan].astype(BF16)
    branch_g = total[:, chan:].astype(BF16).astype(F32)
    branch_x_ref[...] = branch_x
    conv_out = (conv_pre[...] + branch_x.astype(F32) * tap_last[...]).astype(BF16)
    block = recur_weight.shape[1]
    recur, inject = [], []
    for b in range(recur_weight.shape[0]):
        piece = conv_out[:, b * block : (b + 1) * block]
        recur.append(dot(piece, recur_weight[b]))
        inject.append(dot(piece, inject_weight[b]))
    recur_gate = jax.nn.sigmoid(jnp.concatenate(recur, axis=1) + recur_bias[...])
    inject_gate = jax.nn.sigmoid(jnp.concatenate(inject, axis=1) + inject_bias[...])
    neg = -decay_param[...]
    soft = jnp.maximum(neg, 0.0) + jnp.log1p(jnp.exp(-jnp.abs(neg)))
    log_rate = -RATE * recur_gate * soft
    new_state = jnp.exp(log_rate) * lru_state[...] + jnp.sqrt(
        1.0 - jnp.exp(2.0 * log_rate)
    ) * inject_gate * conv_out.astype(F32)
    new_state_ref[...] = new_state
    mix_all[0] = (new_state * jax.nn.gelu(branch_g)).astype(BF16)

    mix_copies = []
    for number, member in enumerate(peers):
        mix_copies.append(
            pltpu.make_async_remote_copy(
                src_ref=mix_all.at[0],
                dst_ref=mix_all.at[number + 1],
                send_sem=mix_send.at[number],
                recv_sem=mix_recv.at[number],
                device_id=there(member),
            )
        )
        mix_copies[-1].start()
    target = lax.broadcasted_iota(jnp.int32, (experts * slots, rows), 0)
    dispatch = jnp.where((target == slot_r0) | (target == slot_r1), 1.0, 0.0).astype(BF16)
    copies[2].wait()
    mixed = tokens[...].astype(F32)
    for number, member in enumerate((t,) + peers):
        if number:
            mix_copies[number - 1].wait_recv()
        span = pl.ds(pl.multiple_of(member * chan, chan), chan)
        mixed += dot(mix_all[number], w_out[span, :])
    stream = mixed.astype(BF16)
    stream_ref[...] = stream
    sorted_rows = dot(dispatch, stream)
    for number in range(experts):
        outbox[number] = sorted_rows[number * slots : (number + 1) * slots].astype(BF16)
    arrived[t, 0] = outbox[e]

    def ep_copy(k):
        to = lax.rem(e + k, experts)
        return pltpu.make_async_remote_copy(
            src_ref=outbox.at[to],
            dst_ref=arrived.at[t, k],
            send_sem=ep_send.at[k],
            recv_sem=ep_recv.at[k],
            device_id={"ep": to},
        )

    def ep_start(k, carry):
        ep_copy(k).start()
        return carry

    lax.fori_loop(1, experts, ep_start, 0)

    def forward(kind, j):
        owner = (t, t, cross)[kind]
        member = (part, cross, part)[kind]
        span = pl.ds(j * GROUP, GROUP)
        return pltpu.make_async_remote_copy(
            src_ref=arrived.at[owner, span],
            dst_ref=arrived.at[owner, span],
            send_sem=fw_send.at[kind, j],
            recv_sem=fw_recv.at[kind, j],
            device_id=there(member),
        )

    def spread(j, carry):
        @pl.when(j < chunks)
        def _():
            for g in range(GROUP):
                k = j * GROUP + g

                @pl.when(k > 0)
                def _():
                    ep_copy(k).wait_recv()

            forward(0, j).start()
            forward(1, j).start()

        @pl.when(j > 0)
        def _():
            forward(1, j - 1).wait_recv()
            forward(2, j - 1).start()

        return carry

    lax.fori_loop(0, chunks + 1, spread, 0)

    for number in (3, 4, 5):
        copies[number].wait()
    hidden_width = w_down.shape[0]

    def p_copy(j):
        return pltpu.make_async_remote_copy(
            src_ref=pbox.at[j],
            dst_ref=pin.at[j],
            send_sem=p_send.at[j],
            recv_sem=p_recv.at[j],
            device_id=there(part),
        )

    def x_copy(j):
        return pltpu.make_async_remote_copy(
            src_ref=xbox.at[j],
            dst_ref=xin.at[j],
            send_sem=x_send.at[j],
            recv_sem=x_recv.at[j],
            device_id=there(cross),
        )

    def r_copy(k):
        to = lax.rem(e - k + experts, experts)
        return pltpu.make_async_remote_copy(
            src_ref=rbox.at[k],
            dst_ref=rin.at[k],
            send_sem=r_send.at[k],
            recv_sem=r_recv.at[k],
            device_id={"ep": to},
        )

    def expert(j, carry):
        @pl.when(j < chunks)
        def _():
            forward(0, j).wait_recv()
            forward(2, j).wait_recv()
            act = jnp.zeros((GROUP * slots, 2 * hidden_width), F32)
            sq = jnp.zeros((GROUP * slots, 1), F32)
            for member in range(4):
                wide = jnp.concatenate(
                    [arrived[member, j * GROUP + g].astype(F32) for g in range(GROUP)], axis=0
                )
                span = pl.ds(member * quarter, quarter)
                sq += jnp.sum(wide * wide, axis=1, keepdims=True)
                act += dot((wide * moe_gain[:, span]).astype(BF16), w_exp[span, :])
            act = act * lax.rsqrt(sq / width + EPS)
            hidden = (jax.nn.silu(act[:, :hidden_width]) * act[:, hidden_width:]).astype(BF16)

            def partial_out(member):
                span = pl.ds(pl.multiple_of(member * quarter, quarter), quarter)
                return dot(hidden, w_down[:, span])

            pbox[j, 0] = partial_out(part).astype(BF16)
            pbox[j, 1] = partial_out(diag).astype(BF16)
            p_copy(j).start()
            keep_own[j] = partial_out(t)
            keep_cross[j] = partial_out(cross)

        @pl.when((j > 0) & (j <= chunks))
        def _():
            p_copy(j - 1).wait_recv()
            xbox[j - 1] = (keep_cross[j - 1] + pin[j - 1, 1].astype(F32)).astype(BF16)
            x_copy(j - 1).start()

        @pl.when(j > 1)
        def _():
            x_copy(j - 2).wait_recv()
            done = keep_own[j - 2] + pin[j - 2, 0].astype(F32) + xin[j - 2].astype(F32)
            for g in range(GROUP):
                k = (j - 2) * GROUP + g
                rbox[k] = done[g * slots : (g + 1) * slots].astype(BF16)

                @pl.when(k > 0)
                def _():
                    r_copy(k).start()

        return carry

    lax.fori_loop(0, chunks + 2, expert, 0)

    lane = lax.broadcasted_iota(jnp.int32, (rows, slots), 1)

    def choose(k):
        first = lax.rem(e + k, experts) * slots
        return jnp.concatenate(
            [
                jnp.where(lane + first == slot_c0, 1.0, 0.0),
                jnp.where(lane + first == slot_c1, 1.0, 0.0),
            ],
            axis=0,
        ).astype(BF16)

    picked[...] = dot(choose(0), rbox[0])

    def gather(k, carry):
        r_copy(k).wait_recv()
        picked[...] += dot(choose(k), rin[k])
        return carry

    lax.fori_loop(1, experts, gather, 0)
    result[...] = (
        stream_ref[...].astype(F32)
        + route_weight[:, 0:1] * picked[:rows]
        + route_weight[:, 1:2] * picked[rows:]
    ).astype(BF16)

    for copy in tok_copies + mix_copies:
        copy.wait_send()

    def drain_ep(k, carry):
        ep_copy(k).wait_send()
        r_copy(k).wait_send()
        return carry

    lax.fori_loop(1, experts, drain_ep, 0)

    def drain_tp(j, carry):
        for kind in range(3):
            forward(kind, j).wait_send()
        p_copy(j).wait_send()
        x_copy(j).wait_send()
        return carry

    lax.fori_loop(0, chunks, drain_tp, 0)


def body(
    tokens,
    conv_state,
    lru_state,
    mix_gain,
    input_weight,
    branch_weight,
    conv_taps,
    conv_bias,
    recur_weight,
    recur_bias,
    inject_weight,
    inject_bias,
    decay_param,
    output_weight,
    moe_gain,
    route_ids,
    route_logits,
    group_weight,
    expert_gate,
    expert_up,
    expert_down,
):
    rows, quarter = tokens.shape
    chan = lru_state.shape[1]
    width = mix_gain.shape[0]
    hidden = expert_gate.shape[2]
    top_count = route_ids.shape[1]
    experts = lax.axis_size("ep")
    tp = lax.axis_size("tp")
    capacity = max(2, min((rows - 2) * top_count // PER_GROUP, 2 * rows * top_count // experts))
    slots = -(-capacity // 8) * 8
    chunks = experts // GROUP
    conv_pre = conv_bias + jnp.sum(conv_state.astype(F32) * conv_taps[None, :-1], axis=1)
    vmem = pl.BlockSpec(memory_space=pltpu.VMEM)
    anywhere = pl.BlockSpec(memory_space=pl.ANY)
    dma = pltpu.SemaphoreType.DMA
    result, new_state, branch_x = pl.pallas_call(
        functools.partial(kernel, experts, slots),
        out_shape=(
            jax.ShapeDtypeStruct((rows, quarter), BF16),
            jax.ShapeDtypeStruct((rows, chan), F32),
            jax.ShapeDtypeStruct((rows, chan), BF16),
        ),
        in_specs=[vmem] * 15 + [anywhere] * 6,
        out_specs=(vmem, vmem, vmem),
        scratch_shapes=[
            pltpu.VMEM((width, 2 * chan), BF16),
            pltpu.VMEM((output_weight.shape[0], quarter), BF16),
            pltpu.VMEM((width, 2 * hidden), BF16),
            pltpu.VMEM((hidden, width), BF16),
            pltpu.VMEM((3, rows, quarter), BF16),
            pltpu.VMEM((4, rows, chan), BF16),
            pltpu.VMEM((rows, quarter), BF16),
            pltpu.VMEM((experts, slots, quarter), BF16),
            pltpu.VMEM((tp, experts, slots, quarter), BF16),
            pltpu.VMEM((chunks, GROUP * slots, quarter), F32),
            pltpu.VMEM((chunks, GROUP * slots, quarter), F32),
            pltpu.VMEM((chunks, 2, GROUP * slots, quarter), BF16),
            pltpu.VMEM((chunks, 2, GROUP * slots, quarter), BF16),
            pltpu.VMEM((chunks, GROUP * slots, quarter), BF16),
            pltpu.VMEM((chunks, GROUP * slots, quarter), BF16),
            pltpu.VMEM((experts, slots, quarter), BF16),
            pltpu.VMEM((experts, slots, quarter), BF16),
            pltpu.VMEM((2 * rows, quarter), F32),
            dma((6,)),
            dma((3,)),
            dma((3,)),
            dma((3,)),
            dma((3,)),
            dma((experts,)),
            dma((experts,)),
            dma((3, chunks)),
            dma((3, chunks)),
            dma((chunks,)),
            dma((chunks,)),
            dma((chunks,)),
            dma((chunks,)),
            dma((experts,)),
            dma((experts,)),
        ],
        compiler_params=pltpu.CompilerParams(collective_id=0, has_side_effects=True),
    )(
        tokens,
        conv_pre,
        lru_state,
        mix_gain[None],
        conv_taps[-1:],
        recur_weight,
        recur_bias[None],
        inject_weight,
        inject_bias[None],
        decay_param[None],
        moe_gain[None],
        route_ids,
        route_ids.T,
        route_logits,
        group_weight[:, None],
        input_weight,
        branch_weight,
        output_weight,
        expert_gate,
        expert_up,
        expert_down,
    )
    new_conv = jnp.concatenate([conv_state[:, 1:], branch_x[:, None, :]], axis=1)
    return (result, new_state, new_conv)


def solution(mesh):
    in_specs = (
        P("ep", "tp"),
        P("ep", None, "tp"),
        P("ep", "tp"),
        P(),
        P(None, "tp"),
        P(None, "tp"),
        P(None, "tp"),
        P("tp"),
        P("tp", None, None),
        P("tp"),
        P("tp", None, None),
        P("tp"),
        P("tp"),
        P(None, "tp"),
        P(),
        P("ep", None),
        P("ep", None),
        P("ep"),
        P("ep", None, "tp"),
        P("ep", None, "tp"),
        P("ep", "tp", None),
    )
    out_specs = (P("ep", "tp"), P("ep", "tp"), P("ep", None, "tp"))
    return jax.shard_map(body, mesh=mesh, in_specs=in_specs, out_specs=out_specs, check_vma=False)
```

```python
import functools

import jax
import jax.numpy as jnp
from jax import lax
from jax.experimental import pallas as pl
from jax.experimental.pallas import tpu as pltpu
from jax.sharding import PartitionSpec as P

PER_GROUP = 4
EPS = 1e-06
RATE = 8.0
GROUP = 2
F32 = jnp.float32
BF16 = jnp.bfloat16


def dot(a, b):
    return jnp.dot(a, b, preferred_element_type=F32)


def kernel(
    experts,
    slots,
    *refs,
):
    (
        tokens_hbm,
        mix_gain_hbm,
        ids_hbm,
        logits_hbm,
        group_hbm,
        input_hbm,
        branch_hbm,
        conv_hbm,
        taps_hbm,
        bias_hbm,
        recur_hbm,
        recur_bias_hbm,
        inject_hbm,
        inject_bias_hbm,
        decay_hbm,
        state_hbm,
        output_hbm,
        moe_gain_hbm,
        gate_hbm,
        up_hbm,
        down_hbm,
        result_hbm,
        new_state_hbm,
        new_conv_hbm,
    ) = refs[:24]
    (
        tokens,
        mix_gain,
        ids_row,
        logits,
        group_weight,
        conv_state,
        conv_taps,
        conv_bias,
        recur_weight,
        recur_bias,
        inject_weight,
        inject_bias,
        decay_param,
        lru_state,
        moe_gain,
        result,
        new_state_ref,
        new_conv,
    ) = refs[24:42]
    (
        w_in,
        w_out,
        w_exp,
        w_down,
        tok_all,
        mix_all,
        stream_ref,
        outbox,
        arrived,
        keep_own,
        keep_cross,
        pbox,
        pin,
        xbox,
        xin,
        rbox,
        rin,
        picked,
        w_sem,
        o_sem,
        tok_send,
        tok_recv,
        mix_send,
        mix_recv,
        ep_send,
        ep_recv,
        fw_send,
        fw_recv,
        p_send,
        p_recv,
        x_send,
        x_recv,
        r_send,
        r_recv,
    ) = refs[42:]
    e = lax.axis_index("ep")
    t = lax.axis_index("tp")
    rows, quarter = tokens.shape
    width = mix_gain.shape[1]
    chan = lru_state.shape[1]
    chunks = experts // GROUP
    part = t + 1 - 2 * (t % 2)
    cross = (t + 2) % 4
    diag = (part + 2) % 4
    peers = (part, cross, diag)

    def there(member):
        return {"tp": member}

    hidden_width = down_hbm.shape[1]
    loads = (
        (tokens_hbm, tokens),
        (mix_gain_hbm, mix_gain),
        (ids_hbm, ids_row),
        (logits_hbm, logits),
        (group_hbm, group_weight),
        (input_hbm, w_in.at[:, pl.ds(0, chan)]),
        (branch_hbm, w_in.at[:, pl.ds(chan, chan)]),
        (conv_hbm, conv_state),
        (taps_hbm, conv_taps),
        (bias_hbm, conv_bias),
        (recur_hbm, recur_weight),
        (recur_bias_hbm, recur_bias),
        (inject_hbm, inject_weight),
        (inject_bias_hbm, inject_bias),
        (decay_hbm, decay_param),
        (state_hbm, lru_state),
        (output_hbm, w_out),
        (moe_gain_hbm, moe_gain),
        (gate_hbm.at[0], w_exp.at[:, pl.ds(0, hidden_width)]),
        (up_hbm.at[0], w_exp.at[:, pl.ds(hidden_width, hidden_width)]),
        (down_hbm.at[0], w_down),
    )
    copies = []
    for number, (source, target) in enumerate(loads):
        copies.append(pltpu.make_async_copy(source, target, w_sem.at[number]))
        copies[-1].start()

    barrier = pltpu.get_barrier_semaphore()
    for member in peers:
        pl.semaphore_signal(barrier, inc=1, device_id=there(member))

    def greet(k, carry):
        pl.semaphore_signal(barrier, inc=1, device_id={"ep": lax.rem(e + k, experts)})
        return carry

    lax.fori_loop(1, experts, greet, 0)
    pl.semaphore_wait(barrier, 3 + experts - 1)

    copies[0].wait()
    tok_copies = []
    for number, member in enumerate(peers):
        tok_copies.append(
            pltpu.make_async_remote_copy(
                src_ref=tokens,
                dst_ref=tok_all.at[number],
                send_sem=tok_send.at[number],
                recv_sem=tok_recv.at[number],
                device_id=there(member),
            )
        )
        tok_copies[-1].start()

    for number in (2, 3, 4):
        copies[number].wait()
    first_r, second_r = ids_row[0:1, :], ids_row[1:2, :]
    row_i = lax.broadcasted_iota(jnp.int32, (rows, rows), 0)
    col_i = lax.broadcasted_iota(jnp.int32, (rows, rows), 1)

    def as_col(row):
        spread_out = jnp.where(row_i == col_i, row.astype(F32), 0.0)
        return jnp.sum(spread_out, axis=1, keepdims=True)

    first_c, second_c = as_col(first_r).astype(jnp.int32), as_col(second_r).astype(jnp.int32)

    def slot_row(mine):
        same = ((first_c == mine) | (second_c == mine)) & (row_i < col_i)
        rank = jnp.sum(jnp.where(same, 1.0, 0.0), axis=0, keepdims=True)
        return mine * slots + rank.astype(jnp.int32)

    def slot_col(mine):
        same = ((first_r == mine) | (second_r == mine)) & (col_i < row_i)
        rank = jnp.sum(jnp.where(same, 1.0, 0.0), axis=1, keepdims=True)
        return mine * slots + rank.astype(jnp.int32)

    slot_r0, slot_r1 = slot_row(first_r), slot_row(second_r)
    slot_c0, slot_c1 = slot_col(first_c), slot_col(second_c)
    raised = jnp.exp(logits[...])
    weight_row = group_weight[...] * raised / jnp.sum(raised, axis=0, keepdims=True)
    weight_0, weight_1 = as_col(weight_row[0:1, :]), as_col(weight_row[1:2, :])

    for number in (1, 5, 6):
        copies[number].wait()
    total = jnp.zeros((rows, 2 * chan), F32)
    squares = jnp.zeros((rows, 1), F32)
    for number, member in enumerate((t,) + peers):
        if number:
            tok_copies[number - 1].wait_recv()
            wide = tok_all[number - 1].astype(F32)
        else:
            wide = tokens[...].astype(F32)
        span = pl.ds(pl.multiple_of(member * quarter, quarter), quarter)
        squares += jnp.sum(wide * wide, axis=1, keepdims=True)
        total += dot((wide * mix_gain[:, span]).astype(BF16), w_in[span, :])
    total = total * lax.rsqrt(squares / width + EPS)
    branch_x = total[:, :chan].astype(BF16)
    branch_g = total[:, chan:].astype(BF16).astype(F32)
    for number in range(7, 16):
        copies[number].wait()
    taps = conv_taps.shape[0]
    conv_sum = conv_bias[...] + branch_x.astype(F32) * conv_taps[taps - 1 : taps, :]
    for tap in range(taps - 1):
        conv_sum += conv_state[tap].astype(F32) * conv_taps[tap : tap + 1, :]
    conv_out = conv_sum.astype(BF16)
    for tap in range(taps - 2):
        new_conv[tap] = conv_state[tap + 1]
    new_conv[taps - 2] = branch_x
    block = recur_weight.shape[1]
    recur, inject = [], []
    for b in range(recur_weight.shape[0]):
        piece = conv_out[:, b * block : (b + 1) * block]
        recur.append(dot(piece, recur_weight[b]))
        inject.append(dot(piece, inject_weight[b]))
    recur_gate = jax.nn.sigmoid(jnp.concatenate(recur, axis=1) + recur_bias[...])
    inject_gate = jax.nn.sigmoid(jnp.concatenate(inject, axis=1) + inject_bias[...])
    neg = -decay_param[...]
    soft = jnp.maximum(neg, 0.0) + jnp.log1p(jnp.exp(-jnp.abs(neg)))
    log_rate = -RATE * recur_gate * soft
    new_state = jnp.exp(log_rate) * lru_state[...] + jnp.sqrt(
        1.0 - jnp.exp(2.0 * log_rate)
    ) * inject_gate * conv_out.astype(F32)
    new_state_ref[...] = new_state
    mix_all[0] = (new_state * jax.nn.gelu(branch_g)).astype(BF16)

    outs = [
        pltpu.make_async_copy(new_state_ref, new_state_hbm, o_sem.at[0]),
        pltpu.make_async_copy(new_conv, new_conv_hbm, o_sem.at[1]),
        pltpu.make_async_copy(result, result_hbm, o_sem.at[2]),
    ]
    mix_copies = []
    for number, member in enumerate(peers):
        mix_copies.append(
            pltpu.make_async_remote_copy(
                src_ref=mix_all.at[0],
                dst_ref=mix_all.at[number + 1],
                send_sem=mix_send.at[number],
                recv_sem=mix_recv.at[number],
                device_id=there(member),
            )
        )
        mix_copies[-1].start()
    outs[0].start()
    outs[1].start()
    target = lax.broadcasted_iota(jnp.int32, (experts * slots, rows), 0)
    dispatch = jnp.where((target == slot_r0) | (target == slot_r1), 1.0, 0.0).astype(BF16)
    copies[16].wait()
    mixed = tokens[...].astype(F32)
    for number, member in enumerate((t,) + peers):
        if number:
            mix_copies[number - 1].wait_recv()
        span = pl.ds(pl.multiple_of(member * chan, chan), chan)
        mixed += dot(mix_all[number], w_out[span, :])
    stream = mixed.astype(BF16)
    stream_ref[...] = stream
    sorted_rows = dot(dispatch, stream)
    for number in range(experts):
        outbox[number] = sorted_rows[number * slots : (number + 1) * slots].astype(BF16)
    arrived[t, 0] = outbox[e]

    def ep_copy(k):
        to = lax.rem(e + k, experts)
        return pltpu.make_async_remote_copy(
            src_ref=outbox.at[to],
            dst_ref=arrived.at[t, k],
            send_sem=ep_send.at[k],
            recv_sem=ep_recv.at[k],
            device_id={"ep": to},
        )

    def ep_start(k, carry):
        ep_copy(k).start()
        return carry

    lax.fori_loop(1, experts, ep_start, 0)

    def forward(kind, j):
        owner = (t, t, cross)[kind]
        member = (part, cross, part)[kind]
        span = pl.ds(j * GROUP, GROUP)
        return pltpu.make_async_remote_copy(
            src_ref=arrived.at[owner, span],
            dst_ref=arrived.at[owner, span],
            send_sem=fw_send.at[kind, j],
            recv_sem=fw_recv.at[kind, j],
            device_id=there(member),
        )

    def spread(j, carry):
        @pl.when(j < chunks)
        def _():
            for g in range(GROUP):
                k = j * GROUP + g

                @pl.when(k > 0)
                def _():
                    ep_copy(k).wait_recv()

            forward(0, j).start()
            forward(1, j).start()

        @pl.when(j > 0)
        def _():
            forward(1, j - 1).wait_recv()
            forward(2, j - 1).start()

        return carry

    lax.fori_loop(0, chunks + 1, spread, 0)

    for number in range(17, 21):
        copies[number].wait()

    def p_copy(j):
        return pltpu.make_async_remote_copy(
            src_ref=pbox.at[j],
            dst_ref=pin.at[j],
            send_sem=p_send.at[j],
            recv_sem=p_recv.at[j],
            device_id=there(part),
        )

    def x_copy(j):
        return pltpu.make_async_remote_copy(
            src_ref=xbox.at[j],
            dst_ref=xin.at[j],
            send_sem=x_send.at[j],
            recv_sem=x_recv.at[j],
            device_id=there(cross),
        )

    def r_copy(k):
        to = lax.rem(e - k + experts, experts)
        return pltpu.make_async_remote_copy(
            src_ref=rbox.at[k],
            dst_ref=rin.at[k],
            send_sem=r_send.at[k],
            recv_sem=r_recv.at[k],
            device_id={"ep": to},
        )

    def expert(j, carry):
        @pl.when(j < chunks)
        def _():
            forward(0, j).wait_recv()
            forward(2, j).wait_recv()
            act = jnp.zeros((GROUP * slots, 2 * hidden_width), F32)
            sq = jnp.zeros((GROUP * slots, 1), F32)
            for member in range(4):
                wide = jnp.concatenate(
                    [arrived[member, j * GROUP + g].astype(F32) for g in range(GROUP)], axis=0
                )
                span = pl.ds(member * quarter, quarter)
                sq += jnp.sum(wide * wide, axis=1, keepdims=True)
                act += dot((wide * moe_gain[:, span]).astype(BF16), w_exp[span, :])
            act = act * lax.rsqrt(sq / width + EPS)
            hidden = (jax.nn.silu(act[:, :hidden_width]) * act[:, hidden_width:]).astype(BF16)

            def partial_out(member):
                span = pl.ds(pl.multiple_of(member * quarter, quarter), quarter)
                return dot(hidden, w_down[:, span])

            pbox[j, 0] = partial_out(part).astype(BF16)
            pbox[j, 1] = partial_out(diag).astype(BF16)
            p_copy(j).start()
            keep_own[j] = partial_out(t)
            keep_cross[j] = partial_out(cross)

        @pl.when((j > 0) & (j <= chunks))
        def _():
            p_copy(j - 1).wait_recv()
            xbox[j - 1] = (keep_cross[j - 1] + pin[j - 1, 1].astype(F32)).astype(BF16)
            x_copy(j - 1).start()

        @pl.when(j > 1)
        def _():
            x_copy(j - 2).wait_recv()
            done = keep_own[j - 2] + pin[j - 2, 0].astype(F32) + xin[j - 2].astype(F32)
            for g in range(GROUP):
                k = (j - 2) * GROUP + g
                rbox[k] = done[g * slots : (g + 1) * slots].astype(BF16)

                @pl.when(k > 0)
                def _():
                    r_copy(k).start()

        return carry

    lax.fori_loop(0, chunks + 2, expert, 0)

    lane = lax.broadcasted_iota(jnp.int32, (rows, slots), 1)

    def choose(k):
        first = lax.rem(e + k, experts) * slots
        return jnp.concatenate(
            [
                jnp.where(lane + first == slot_c0, 1.0, 0.0),
                jnp.where(lane + first == slot_c1, 1.0, 0.0),
            ],
            axis=0,
        ).astype(BF16)

    picked[...] = dot(choose(0), rbox[0])

    def gather(k, carry):
        r_copy(k).wait_recv()
        picked[...] += dot(choose(k), rin[k])
        return carry

    lax.fori_loop(1, experts, gather, 0)
    result[...] = (
        stream_ref[...].astype(F32)
        + weight_0 * picked[:rows]
        + weight_1 * picked[rows:]
    ).astype(BF16)

    outs[2].start()

    for copy in tok_copies + mix_copies:
        copy.wait_send()
    for copy in outs:
        copy.wait()

    def drain_ep(k, carry):
        ep_copy(k).wait_send()
        r_copy(k).wait_send()
        return carry

    lax.fori_loop(1, experts, drain_ep, 0)

    def drain_tp(j, carry):
        for kind in range(3):
            forward(kind, j).wait_send()
        p_copy(j).wait_send()
        x_copy(j).wait_send()
        return carry

    lax.fori_loop(0, chunks, drain_tp, 0)


def body(
    tokens,
    conv_state,
    lru_state,
    mix_gain,
    input_weight,
    branch_weight,
    conv_taps,
    conv_bias,
    recur_weight,
    recur_bias,
    inject_weight,
    inject_bias,
    decay_param,
    output_weight,
    moe_gain,
    route_ids,
    route_logits,
    group_weight,
    expert_gate,
    expert_up,
    expert_down,
):
    rows, quarter = tokens.shape
    chan = lru_state.shape[1]
    width = mix_gain.shape[0]
    hidden = expert_gate.shape[2]
    top_count = route_ids.shape[1]
    experts = lax.axis_size("ep")
    tp = lax.axis_size("tp")
    capacity = max(2, min((rows - 2) * top_count // PER_GROUP, 2 * rows * top_count // experts))
    slots = -(-capacity // 8) * 8
    chunks = experts // GROUP
    anywhere = pl.BlockSpec(memory_space=pl.ANY)
    dma = pltpu.SemaphoreType.DMA
    result, new_state, new_conv = pl.pallas_call(
        functools.partial(kernel, experts, slots),
        out_shape=(
            jax.ShapeDtypeStruct((rows, quarter), BF16),
            jax.ShapeDtypeStruct((rows, chan), F32),
            jax.ShapeDtypeStruct((conv_taps.shape[0] - 1, rows, chan), BF16),
        ),
        in_specs=[anywhere] * 21,
        out_specs=(anywhere, anywhere, anywhere),
        scratch_shapes=[
            pltpu.VMEM((rows, quarter), BF16),
            pltpu.VMEM((1, width), F32),
            pltpu.VMEM((top_count, rows), jnp.int32),
            pltpu.VMEM((top_count, rows), F32),
            pltpu.VMEM((1, rows), F32),
            pltpu.VMEM((conv_taps.shape[0] - 1, rows, chan), BF16),
            pltpu.VMEM(conv_taps.shape, F32),
            pltpu.VMEM((1, chan), F32),
            pltpu.VMEM(recur_weight.shape, BF16),
            pltpu.VMEM((1, chan), F32),
            pltpu.VMEM(inject_weight.shape, BF16),
            pltpu.VMEM((1, chan), F32),
            pltpu.VMEM((1, chan), F32),
            pltpu.VMEM((rows, chan), F32),
            pltpu.VMEM((1, width), F32),
            pltpu.VMEM((rows, quarter), BF16),
            pltpu.VMEM((rows, chan), F32),
            pltpu.VMEM((conv_taps.shape[0] - 1, rows, chan), BF16),
            pltpu.VMEM((width, 2 * chan), BF16),
            pltpu.VMEM((output_weight.shape[0], quarter), BF16),
            pltpu.VMEM((width, 2 * hidden), BF16),
            pltpu.VMEM((hidden, width), BF16),
            pltpu.VMEM((3, rows, quarter), BF16),
            pltpu.VMEM((4, rows, chan), BF16),
            pltpu.VMEM((rows, quarter), BF16),
            pltpu.VMEM((experts, slots, quarter), BF16),
            pltpu.VMEM((tp, experts, slots, quarter), BF16),
            pltpu.VMEM((chunks, GROUP * slots, quarter), F32),
            pltpu.VMEM((chunks, GROUP * slots, quarter), F32),
            pltpu.VMEM((chunks, 2, GROUP * slots, quarter), BF16),
            pltpu.VMEM((chunks, 2, GROUP * slots, quarter), BF16),
            pltpu.VMEM((chunks, GROUP * slots, quarter), BF16),
            pltpu.VMEM((chunks, GROUP * slots, quarter), BF16),
            pltpu.VMEM((experts, slots, quarter), BF16),
            pltpu.VMEM((experts, slots, quarter), BF16),
            pltpu.VMEM((2 * rows, quarter), F32),
            dma((21,)),
            dma((3,)),
            dma((3,)),
            dma((3,)),
            dma((3,)),
            dma((3,)),
            dma((experts,)),
            dma((experts,)),
            dma((3, chunks)),
            dma((3, chunks)),
            dma((chunks,)),
            dma((chunks,)),
            dma((chunks,)),
            dma((chunks,)),
            dma((experts,)),
            dma((experts,)),
        ],
        compiler_params=pltpu.CompilerParams(collective_id=0, has_side_effects=True),
    )(
        tokens,
        mix_gain[None],
        route_ids.T,
        route_logits.T,
        group_weight[None],
        input_weight,
        branch_weight,
        conv_state.transpose(1, 0, 2),
        conv_taps,
        conv_bias[None],
        recur_weight,
        recur_bias[None],
        inject_weight,
        inject_bias[None],
        decay_param[None],
        lru_state,
        output_weight,
        moe_gain[None],
        expert_gate,
        expert_up,
        expert_down,
    )
    return (result, new_state, new_conv.transpose(1, 0, 2))


def solution(mesh):
    in_specs = (
        P("ep", "tp"),
        P("ep", None, "tp"),
        P("ep", "tp"),
        P(),
        P(None, "tp"),
        P(None, "tp"),
        P(None, "tp"),
        P("tp"),
        P("tp", None, None),
        P("tp"),
        P("tp", None, None),
        P("tp"),
        P("tp"),
        P(None, "tp"),
        P(),
        P("ep", None),
        P("ep", None),
        P("ep"),
        P("ep", None, "tp"),
        P("ep", None, "tp"),
        P("ep", "tp", None),
    )
    out_specs = (P("ep", "tp"), P("ep", "tp"), P("ep", None, "tp"))
    return jax.shard_map(body, mesh=mesh, in_specs=in_specs, out_specs=out_specs, check_vma=False)
```

```python
import functools

import jax
import jax.numpy as jnp
from jax import lax
from jax.experimental import pallas as pl
from jax.experimental.pallas import tpu as pltpu
from jax.sharding import PartitionSpec as P

PER_GROUP = 4
EPS = 1e-06
RATE = 8.0
GROUP = 2
F32 = jnp.float32
BF16 = jnp.bfloat16


def dot(a, b):
    return jnp.dot(a, b, preferred_element_type=F32)


def kernel(
    experts,
    slots,
    *refs,
):
    (
        tokens_hbm,
        mix_gain_hbm,
        ids_hbm,
        logits_hbm,
        group_hbm,
        input_hbm,
        branch_hbm,
        conv_hbm,
        taps_hbm,
        bias_hbm,
        recur_hbm,
        recur_bias_hbm,
        inject_hbm,
        inject_bias_hbm,
        decay_hbm,
        state_hbm,
        output_hbm,
        moe_gain_hbm,
        gate_hbm,
        up_hbm,
        down_hbm,
        result,
        new_state_ref,
        new_conv,
    ) = refs[:24]
    (
        tokens,
        mix_gain,
        ids_row,
        logits,
        group_weight,
        conv_state,
        conv_taps,
        conv_bias,
        recur_weight,
        recur_bias,
        inject_weight,
        inject_bias,
        decay_param,
        lru_state,
        moe_gain,
    ) = refs[24:39]
    (
        w_in,
        w_out,
        w_exp,
        w_down,
        tok_all,
        mix_all,
        stream_ref,
        outbox,
        arrived,
        keep_own,
        keep_cross,
        pbox,
        pin,
        xbox,
        xin,
        rbox,
        rin,
        picked,
        w_sem,
        tok_send,
        tok_recv,
        mix_send,
        mix_recv,
        ep_send,
        ep_recv,
        fw_send,
        fw_recv,
        p_send,
        p_recv,
        x_send,
        x_recv,
        r_send,
        r_recv,
    ) = refs[39:]
    e = lax.axis_index("ep")
    t = lax.axis_index("tp")
    rows, quarter = tokens.shape
    width = mix_gain.shape[1]
    chan = lru_state.shape[1]
    chunks = experts // GROUP
    part = t + 1 - 2 * (t % 2)
    cross = (t + 2) % 4
    diag = (part + 2) % 4
    peers = (part, cross, diag)

    def there(member):
        return {"tp": member}

    hidden_width = down_hbm.shape[1]
    loads = (
        (tokens_hbm, tokens),
        (mix_gain_hbm, mix_gain),
        (ids_hbm, ids_row),
        (logits_hbm, logits),
        (group_hbm, group_weight),
        (input_hbm, w_in.at[:, pl.ds(0, chan)]),
        (branch_hbm, w_in.at[:, pl.ds(chan, chan)]),
        (conv_hbm, conv_state),
        (taps_hbm, conv_taps),
        (bias_hbm, conv_bias),
        (recur_hbm, recur_weight),
        (recur_bias_hbm, recur_bias),
        (inject_hbm, inject_weight),
        (inject_bias_hbm, inject_bias),
        (decay_hbm, decay_param),
        (state_hbm, lru_state),
        (output_hbm, w_out),
        (moe_gain_hbm, moe_gain),
        (gate_hbm.at[0], w_exp.at[:, pl.ds(0, hidden_width)]),
        (up_hbm.at[0], w_exp.at[:, pl.ds(hidden_width, hidden_width)]),
        (down_hbm.at[0], w_down),
    )
    copies = []
    for number, (source, target) in enumerate(loads):
        copies.append(pltpu.make_async_copy(source, target, w_sem.at[number]))
        copies[-1].start()

    barrier = pltpu.get_barrier_semaphore()
    for member in peers:
        pl.semaphore_signal(barrier, inc=1, device_id=there(member))

    def greet(k, carry):
        pl.semaphore_signal(barrier, inc=1, device_id={"ep": lax.rem(e + k, experts)})
        return carry

    lax.fori_loop(1, experts, greet, 0)
    pl.semaphore_wait(barrier, 3 + experts - 1)

    copies[0].wait()
    tok_copies = []
    for number, member in enumerate(peers):
        tok_copies.append(
            pltpu.make_async_remote_copy(
                src_ref=tokens,
                dst_ref=tok_all.at[number],
                send_sem=tok_send.at[number],
                recv_sem=tok_recv.at[number],
                device_id=there(member),
            )
        )
        tok_copies[-1].start()

    for number in (2, 3, 4):
        copies[number].wait()
    first_r, second_r = ids_row[0:1, :], ids_row[1:2, :]
    row_i = lax.broadcasted_iota(jnp.int32, (rows, rows), 0)
    col_i = lax.broadcasted_iota(jnp.int32, (rows, rows), 1)

    def as_col(row):
        spread_out = jnp.where(row_i == col_i, row.astype(F32), 0.0)
        return jnp.sum(spread_out, axis=1, keepdims=True)

    first_c, second_c = as_col(first_r).astype(jnp.int32), as_col(second_r).astype(jnp.int32)

    def slot_row(mine):
        same = ((first_c == mine) | (second_c == mine)) & (row_i < col_i)
        rank = jnp.sum(jnp.where(same, 1.0, 0.0), axis=0, keepdims=True)
        return mine * slots + rank.astype(jnp.int32)

    def slot_col(mine):
        same = ((first_r == mine) | (second_r == mine)) & (col_i < row_i)
        rank = jnp.sum(jnp.where(same, 1.0, 0.0), axis=1, keepdims=True)
        return mine * slots + rank.astype(jnp.int32)

    slot_r0, slot_r1 = slot_row(first_r), slot_row(second_r)
    slot_c0, slot_c1 = slot_col(first_c), slot_col(second_c)
    raised = jnp.exp(logits[...])
    weight_row = group_weight[...] * raised / jnp.sum(raised, axis=0, keepdims=True)
    weight_0, weight_1 = as_col(weight_row[0:1, :]), as_col(weight_row[1:2, :])

    for number in (1, 5, 6):
        copies[number].wait()
    total = jnp.zeros((rows, 2 * chan), F32)
    squares = jnp.zeros((rows, 1), F32)
    for number, member in enumerate((t,) + peers):
        if number:
            tok_copies[number - 1].wait_recv()
            wide = tok_all[number - 1].astype(F32)
        else:
            wide = tokens[...].astype(F32)
        span = pl.ds(pl.multiple_of(member * quarter, quarter), quarter)
        squares += jnp.sum(wide * wide, axis=1, keepdims=True)
        total += dot((wide * mix_gain[:, span]).astype(BF16), w_in[span, :])
    total = total * lax.rsqrt(squares / width + EPS)
    branch_x = total[:, :chan].astype(BF16)
    branch_g = total[:, chan:].astype(BF16).astype(F32)
    for number in range(7, 16):
        copies[number].wait()
    taps = conv_taps.shape[0]
    conv_sum = conv_bias[...] + branch_x.astype(F32) * conv_taps[taps - 1 : taps, :]
    for tap in range(taps - 1):
        conv_sum += conv_state[tap].astype(F32) * conv_taps[tap : tap + 1, :]
    conv_out = conv_sum.astype(BF16)
    for tap in range(taps - 2):
        new_conv[tap] = conv_state[tap + 1]
    new_conv[taps - 2] = branch_x
    block = recur_weight.shape[1]
    recur, inject = [], []
    for b in range(recur_weight.shape[0]):
        piece = conv_out[:, b * block : (b + 1) * block]
        recur.append(dot(piece, recur_weight[b]))
        inject.append(dot(piece, inject_weight[b]))
    recur_gate = jax.nn.sigmoid(jnp.concatenate(recur, axis=1) + recur_bias[...])
    inject_gate = jax.nn.sigmoid(jnp.concatenate(inject, axis=1) + inject_bias[...])
    neg = -decay_param[...]
    soft = jnp.maximum(neg, 0.0) + jnp.log1p(jnp.exp(-jnp.abs(neg)))
    log_rate = -RATE * recur_gate * soft
    new_state = jnp.exp(log_rate) * lru_state[...] + jnp.sqrt(
        1.0 - jnp.exp(2.0 * log_rate)
    ) * inject_gate * conv_out.astype(F32)
    new_state_ref[...] = new_state
    mix_all[0] = (new_state * jax.nn.gelu(branch_g)).astype(BF16)

    mix_copies = []
    for number, member in enumerate(peers):
        mix_copies.append(
            pltpu.make_async_remote_copy(
                src_ref=mix_all.at[0],
                dst_ref=mix_all.at[number + 1],
                send_sem=mix_send.at[number],
                recv_sem=mix_recv.at[number],
                device_id=there(member),
            )
        )
        mix_copies[-1].start()
    target = lax.broadcasted_iota(jnp.int32, (experts * slots, rows), 0)
    dispatch = jnp.where((target == slot_r0) | (target == slot_r1), 1.0, 0.0).astype(BF16)
    copies[16].wait()
    mixed = tokens[...].astype(F32)
    for number, member in enumerate((t,) + peers):
        if number:
            mix_copies[number - 1].wait_recv()
        span = pl.ds(pl.multiple_of(member * chan, chan), chan)
        mixed += dot(mix_all[number], w_out[span, :])
    stream = mixed.astype(BF16)
    stream_ref[...] = stream
    sorted_rows = dot(dispatch, stream)
    for number in range(experts):
        outbox[number] = sorted_rows[number * slots : (number + 1) * slots].astype(BF16)
    arrived[t, 0] = outbox[e]

    def ep_copy(k):
        to = lax.rem(e + k, experts)
        return pltpu.make_async_remote_copy(
            src_ref=outbox.at[to],
            dst_ref=arrived.at[t, k],
            send_sem=ep_send.at[k],
            recv_sem=ep_recv.at[k],
            device_id={"ep": to},
        )

    def ep_start(k, carry):
        ep_copy(experts - k).start()
        return carry

    lax.fori_loop(1, experts, ep_start, 0)

    def forward(kind, j):
        owner = (t, t, cross)[kind]
        member = (part, cross, part)[kind]
        span = pl.ds(j * GROUP, GROUP)
        return pltpu.make_async_remote_copy(
            src_ref=arrived.at[owner, span],
            dst_ref=arrived.at[owner, span],
            send_sem=fw_send.at[kind, j],
            recv_sem=fw_recv.at[kind, j],
            device_id=there(member),
        )

    last = chunks - 1

    def spread(j):
        @pl.when(j < chunks)
        def _():
            for g in range(GROUP):
                k = (last - j) * GROUP + g

                @pl.when(k > 0)
                def _():
                    ep_copy(k).wait_recv()

            forward(0, last - j).start()
            forward(1, last - j).start()

        @pl.when((j > 0) & (j <= chunks))
        def _():
            forward(1, last - j + 1).wait_recv()
            forward(2, last - j + 1).start()

    for number in range(17, 21):
        copies[number].wait()

    def p_copy(j):
        return pltpu.make_async_remote_copy(
            src_ref=pbox.at[j],
            dst_ref=pin.at[j],
            send_sem=p_send.at[j],
            recv_sem=p_recv.at[j],
            device_id=there(part),
        )

    def x_copy(j):
        return pltpu.make_async_remote_copy(
            src_ref=xbox.at[j],
            dst_ref=xin.at[j],
            send_sem=x_send.at[j],
            recv_sem=x_recv.at[j],
            device_id=there(cross),
        )

    def r_copy(k):
        to = lax.rem(e - k + experts, experts)
        return pltpu.make_async_remote_copy(
            src_ref=rbox.at[k],
            dst_ref=rin.at[k],
            send_sem=r_send.at[k],
            recv_sem=r_recv.at[k],
            device_id={"ep": to},
        )

    def expert(step, carry):
        spread(step)
        j = step - 2

        @pl.when((j >= 0) & (j < chunks))
        def _():
            b = last - j
            forward(0, b).wait_recv()
            forward(2, b).wait_recv()
            act = jnp.zeros((GROUP * slots, 2 * hidden_width), F32)
            sq = jnp.zeros((GROUP * slots, 1), F32)
            for member in range(4):
                wide = jnp.concatenate(
                    [arrived[member, b * GROUP + g].astype(F32) for g in range(GROUP)], axis=0
                )
                span = pl.ds(member * quarter, quarter)
                sq += jnp.sum(wide * wide, axis=1, keepdims=True)
                act += dot((wide * moe_gain[:, span]).astype(BF16), w_exp[span, :])
            act = act * lax.rsqrt(sq / width + EPS)
            hidden = (jax.nn.silu(act[:, :hidden_width]) * act[:, hidden_width:]).astype(BF16)

            def partial_out(member):
                span = pl.ds(pl.multiple_of(member * quarter, quarter), quarter)
                return dot(hidden, w_down[:, span])

            pbox[b, 0] = partial_out(part).astype(BF16)
            pbox[b, 1] = partial_out(diag).astype(BF16)
            p_copy(b).start()
            keep_own[b] = partial_out(t)
            keep_cross[b] = partial_out(cross)

        @pl.when((j > 0) & (j <= chunks))
        def _():
            b = last - j + 1
            p_copy(b).wait_recv()
            xbox[b] = (keep_cross[b] + pin[b, 1].astype(F32)).astype(BF16)
            x_copy(b).start()

        @pl.when(j > 2)
        def _():
            b = last - j + 3
            x_copy(b).wait_recv()
            done = keep_own[b] + pin[b, 0].astype(F32) + xin[b].astype(F32)
            for g in range(GROUP):
                k = b * GROUP + g
                rbox[k] = done[g * slots : (g + 1) * slots].astype(BF16)

                @pl.when(k > 0)
                def _():
                    r_copy(k).start()

        return carry

    lax.fori_loop(0, chunks + 5, expert, 0)

    lane = lax.broadcasted_iota(jnp.int32, (rows, slots), 1)

    def choose(k):
        first = lax.rem(e + k, experts) * slots
        return jnp.concatenate(
            [
                jnp.where(lane + first == slot_c0, 1.0, 0.0),
                jnp.where(lane + first == slot_c1, 1.0, 0.0),
            ],
            axis=0,
        ).astype(BF16)

    picked[...] = dot(choose(0), rbox[0])

    def gather(step, carry):
        k = experts - step
        r_copy(k).wait_recv()
        picked[...] += dot(choose(k), rin[k])
        return carry

    lax.fori_loop(1, experts, gather, 0)
    result[...] = (
        stream_ref[...].astype(F32)
        + weight_0 * picked[:rows]
        + weight_1 * picked[rows:]
    ).astype(BF16)


    for copy in tok_copies + mix_copies:
        copy.wait_send()

    def drain_ep(k, carry):
        ep_copy(k).wait_send()
        r_copy(k).wait_send()
        return carry

    lax.fori_loop(1, experts, drain_ep, 0)

    def drain_tp(j, carry):
        for kind in range(3):
            forward(kind, j).wait_send()
        p_copy(j).wait_send()
        x_copy(j).wait_send()
        return carry

    lax.fori_loop(0, chunks, drain_tp, 0)


def body(
    tokens,
    conv_state,
    lru_state,
    mix_gain,
    input_weight,
    branch_weight,
    conv_taps,
    conv_bias,
    recur_weight,
    recur_bias,
    inject_weight,
    inject_bias,
    decay_param,
    output_weight,
    moe_gain,
    route_ids,
    route_logits,
    group_weight,
    expert_gate,
    expert_up,
    expert_down,
):
    rows, quarter = tokens.shape
    chan = lru_state.shape[1]
    width = mix_gain.shape[0]
    hidden = expert_gate.shape[2]
    top_count = route_ids.shape[1]
    experts = lax.axis_size("ep")
    tp = lax.axis_size("tp")
    capacity = max(2, min((rows - 2) * top_count // PER_GROUP, 2 * rows * top_count // experts))
    slots = -(-capacity // 8) * 8
    chunks = experts // GROUP
    vmem = pl.BlockSpec(memory_space=pltpu.VMEM)
    anywhere = pl.BlockSpec(memory_space=pl.ANY)
    dma = pltpu.SemaphoreType.DMA
    shapes = (
        jax.ShapeDtypeStruct((rows, quarter), BF16),
        jax.ShapeDtypeStruct((rows, chan), F32),
        jax.ShapeDtypeStruct((conv_taps.shape[0] - 1, rows, chan), BF16),
    )
    made = pl.pallas_call(
        functools.partial(kernel, experts, slots),
        out_shape=tuple(pltpu.VMEM(s.shape, s.dtype) for s in shapes),
        in_specs=[anywhere] * 21,
        out_specs=(vmem, vmem, vmem),
        scratch_shapes=[
            pltpu.VMEM((rows, quarter), BF16),
            pltpu.VMEM((1, width), F32),
            pltpu.VMEM((top_count, rows), jnp.int32),
            pltpu.VMEM((top_count, rows), F32),
            pltpu.VMEM((1, rows), F32),
            pltpu.VMEM((conv_taps.shape[0] - 1, rows, chan), BF16),
            pltpu.VMEM(conv_taps.shape, F32),
            pltpu.VMEM((1, chan), F32),
            pltpu.VMEM(recur_weight.shape, BF16),
            pltpu.VMEM((1, chan), F32),
            pltpu.VMEM(inject_weight.shape, BF16),
            pltpu.VMEM((1, chan), F32),
            pltpu.VMEM((1, chan), F32),
            pltpu.VMEM((rows, chan), F32),
            pltpu.VMEM((1, width), F32),
            pltpu.VMEM((width, 2 * chan), BF16),
            pltpu.VMEM((output_weight.shape[0], quarter), BF16),
            pltpu.VMEM((width, 2 * hidden), BF16),
            pltpu.VMEM((hidden, width), BF16),
            pltpu.VMEM((3, rows, quarter), BF16),
            pltpu.VMEM((4, rows, chan), BF16),
            pltpu.VMEM((rows, quarter), BF16),
            pltpu.VMEM((experts, slots, quarter), BF16),
            pltpu.VMEM((tp, experts, slots, quarter), BF16),
            pltpu.VMEM((chunks, GROUP * slots, quarter), F32),
            pltpu.VMEM((chunks, GROUP * slots, quarter), F32),
            pltpu.VMEM((chunks, 2, GROUP * slots, quarter), BF16),
            pltpu.VMEM((chunks, 2, GROUP * slots, quarter), BF16),
            pltpu.VMEM((chunks, GROUP * slots, quarter), BF16),
            pltpu.VMEM((chunks, GROUP * slots, quarter), BF16),
            pltpu.VMEM((experts, slots, quarter), BF16),
            pltpu.VMEM((experts, slots, quarter), BF16),
            pltpu.VMEM((2 * rows, quarter), F32),
            dma((21,)),
            dma((3,)),
            dma((3,)),
            dma((3,)),
            dma((3,)),
            dma((experts,)),
            dma((experts,)),
            dma((3, chunks)),
            dma((3, chunks)),
            dma((chunks,)),
            dma((chunks,)),
            dma((chunks,)),
            dma((chunks,)),
            dma((experts,)),
            dma((experts,)),
        ],
        compiler_params=pltpu.CompilerParams(collective_id=0, has_side_effects=True),
    )(
        tokens,
        mix_gain[None],
        route_ids.T,
        route_logits.T,
        group_weight[None],
        input_weight,
        branch_weight,
        conv_state.transpose(1, 0, 2),
        conv_taps,
        conv_bias[None],
        recur_weight,
        recur_bias[None],
        inject_weight,
        inject_bias[None],
        decay_param[None],
        lru_state,
        output_weight,
        moe_gain[None],
        expert_gate,
        expert_up,
        expert_down,
    )
    result, new_state, new_conv = made
    return (result, new_state, new_conv.transpose(1, 0, 2))


def solution(mesh):
    in_specs = (
        P("ep", "tp"),
        P("ep", None, "tp"),
        P("ep", "tp"),
        P(),
        P(None, "tp"),
        P(None, "tp"),
        P(None, "tp"),
        P("tp"),
        P("tp", None, None),
        P("tp"),
        P("tp", None, None),
        P("tp"),
        P("tp"),
        P(None, "tp"),
        P(),
        P("ep", None),
        P("ep", None),
        P("ep"),
        P("ep", None, "tp"),
        P("ep", None, "tp"),
        P("ep", "tp", None),
    )
    out_specs = (P("ep", "tp"), P("ep", "tp"), P("ep", None, "tp"))
    return jax.shard_map(body, mesh=mesh, in_specs=in_specs, out_specs=out_specs, check_vma=False)
```
